512 devices in a mesh: ep: 32 (over z, core), tp: 16 (over y, x).
Axes of the slice: x: 4, y: 4, z: 16, core: 2. Of those that a mesh axis runs over, the one named last changes fastest.
Arguments:
- compressed_query: bfloat16 [4096, 1536], P('ep'), may hold values from -6 to 6
- compressed_key_value: bfloat16 [4096, 512], P('ep'), may hold values from -6 to 6
- rotary_key: bfloat16 [4096, 32], P('ep'), may hold values from -600 to 600
- query_norm_scale: float32 [1536], replicated, may hold values from 0.1 to 1.9
- context_norm_scale: float32 [512], replicated, may hold values from 0.1 to 1.9
- query_plain_weight: bfloat16 [1536, 1024], P(None, 'tp'), may hold values from -0.375 to 0.375
- query_rotary_weight: bfloat16 [1536, 512], P(None, 'tp'), may hold values from -0.375 to 0.375
- key_up_weight: bfloat16 [512, 1024], P(None, 'tp'), may hold values from -0.25 to 0.25
- value_up_weight: bfloat16 [512, 1024], P(None, 'tp'), may hold values from -0.25 to 0.25
- output_weight: bfloat16 [1024, 2048], P(None, 'tp'), may hold values from -0.75 to 0.75
- mixture_input: bfloat16 [4096, 2048], P('ep'), may hold values from -6 to 6
- mixture_gain: float32 [2048], replicated, may hold values from 0.1 to 1.9
- routes: int32 [4096, 2], P('ep'), may hold values from 0 to 31, all different within a row; in each aligned block of 128 rows (0 to 127, 128 to 255, ...) at most 12 rows name the same one
- route_weight: float32 [4096, 2], P('ep'), may hold values from 0.2 to 2
- expert_gate: bfloat16 [32, 2048, 4096], P('ep', None, 'tp'), may hold values from -0.125 to 0.125
- expert_up: bfloat16 [32, 2048, 4096], P('ep', None, 'tp'), may hold values from -0.125 to 0.125
- expert_down: bfloat16 [32, 4096, 2048], P('ep', None, 'tp'), may hold values from -0.09375 to 0.09375
- shared_gate: bfloat16 [2048, 512], P(None, 'tp'), may hold values from -0.125 to 0.125
- shared_up: bfloat16 [2048, 512], P(None, 'tp'), may hold values from -0.125 to 0.125
- shared_down: bfloat16 [512, 2048], P(None, 'tp'), may hold values from -0.25 to 0.25
Outputs:
- attended: bfloat16 [4096, 2048], P('ep', 'tp')
- combined: bfloat16 [4096, 2048], P('ep', 'tp')
The draws below stay inside these ranges and needn't reach their ends.
Inputs may be any that keep to these rules, and one draw needn't show every extreme that they name: `routes`: in the rows of each index of ep, no expert is named more than 12 times, a bound that some block reaches there.
All inputs are finite; a program needn't handle non-finite values.
Results may differ from the reference program's by a relative error of at most 0.012.
The reference program's roundings to bfloat16 on the way count: a program that leaves them out, or rounds other values in their place, can miss the bound.
Values may be sent and summed in bfloat16 or wider, within the bound.
No kernel may reach another device: no remote copies, remote signals or barrier semaphores. Data moves between devices by JAX's collectives and lax.ppermute only.
A program may use at most 64 MiB of HBM per device.

```python
import math
import jax
import jax.numpy as jnp
import numpy as np
from jax import lax

D = 2048
HEAD_COUNT = 16
PLAIN_HEAD_SIZE = 64
ROTARY_SIZE = 32
VALUE_HEAD_SIZE = 64
QUERY_RANK = 1536
KEY_VALUE_RANK = 512
EXP_FF = 4096
SH_FF = 512
TOPK = 2
TOK2 = 128
SEQUENCE_LEN1 = 4096
TOKENS2 = 4096
EXPERTS = 32
CAP = 12
N_EP = 32


def draw_rotary_key(key, part):
    base = jax.random.normal(key, (SEQUENCE_LEN1, ROTARY_SIZE), jnp.float32)
    return base.astype(jnp.bfloat16)


def levels(rng, extent, pieces, least, high):
    loudness, own = 1.0, jax.random.fold_in(rng, 6)
    for dim, parts in pieces:
        heights = jnp.exp(jax.random.uniform(jax.random.fold_in(own, dim), (parts,), jnp.float32, least / len(pieces), high / len(pieces)))
        loudness = loudness * jnp.repeat(heights, extent[dim] // parts).reshape([-1 if axis == dim else 1 for axis in range(len(extent))])
    return loudness


def assign_block(rng, own, number, rows, number_of, top, most, lean):
    order = jax.random.permutation(rng, number_of)
    packed, common = load_shares(number_of, rows * top, most, lean, True), load_shares(number_of, rows * top, most, lean, False)
    places = jnp.arange(number_of)

    def named(tallies, offset_by):
        used = int((tallies > 0).sum())
        fixed = max(1, used // 4)
        moved = fixed + (places - fixed + offset_by * (used - fixed)) % max(1, number_of - fixed)
        return jnp.zeros((number_of,), jnp.int32).at[order[jnp.where(places < fixed, places, moved)]].set(jnp.asarray(tallies, jnp.int32))

    tallies = jnp.where(number % 4 == 0, named(packed, number // 4), named(common, number - number // 4 - 1))
    mixed = jax.random.permutation(jax.random.fold_in(own, 3), number_of)
    donor, sink = mixed[0:number_of // 2 * 2:2], mixed[1:number_of // 2 * 2:2]
    room = jnp.minimum(tallies[donor] - 1, most - tallies[sink]) // 2
    room = jnp.where((donor == order[0]) | (sink == order[0]) | (tallies[sink] == 0), 0, jnp.maximum(room, 0))
    moved = jax.random.randint(jax.random.fold_in(own, 4), (number_of // 2,), 0, 1 << 20) % (room + 1)
    tallies = tallies.at[donor].add(-moved).at[sink].add(moved)
    members = jnp.searchsorted(jnp.cumsum(tallies), jnp.arange(rows * top), side="right").astype(jnp.int32)
    listing = members.reshape(top, rows).T
    listing = listing[jax.random.permutation(jax.random.fold_in(own, 1), rows)]
    offset_by = jax.random.randint(jax.random.fold_in(own, 2), (rows, 1), 0, top)
    return jnp.take_along_axis(listing, (jnp.arange(top)[None, :] + offset_by) % top, axis=1)


def load_shares(count, total, limit, slope, full):
    loads = [(1 << 20) // math.isqrt(grade ** slope) + 1 for grade in range(1, count + 1)]
    largest = limit if full else min(limit, max(-(-total // count), total * loads[0] // sum(loads)))
    least = 1 if total - largest >= count - 1 else 0
    given, surplus = [largest] + [least] * (count - 1), total - largest - least * (count - 1)
    while surplus > 0:
        candidates = [i for i in range(1, count) if given[i] < largest] or [i for i in range(1, count) if given[i] < limit]
        pool, remaining = sum([loads[i] for i in candidates]), surplus
        for i in candidates:
            addition = min(limit - given[i], max(1, remaining * loads[i] // pool), surplus)
            given[i] = given[i] + addition
            surplus = surplus - addition
    return np.array(given)


def noise(own_key, extent, deviation, bound, cuts=(), kind=jnp.bfloat16):
    factor_of = levels(own_key, extent, cuts, -0.22, 0.18) if cuts else 1.0
    result = jax.random.normal(own_key, extent, jnp.float32) * deviation * factor_of
    return jnp.minimum(jnp.maximum(result, -bound), bound).astype(kind)


def setup_inputs(seed: int = 0) -> dict:
    arg_keys = jax.random.split(jax.random.key(seed), 21)
    compressed_query = noise(arg_keys[0], (SEQUENCE_LEN1, QUERY_RANK), 1.0, 6.0, ((0, 32),))
    compressed_key_value = noise(arg_keys[1], (SEQUENCE_LEN1, KEY_VALUE_RANK), 1.0, 6.0, ((0, 32),))
    rotary_key = draw_rotary_key(jax.random.fold_in(arg_keys[20], 71), 0)
    query_norm_scale = jnp.clip(1.0 + 0.18 * jax.random.normal(arg_keys[3], (QUERY_RANK,), jnp.float32), 0.1, 1.9)
    context_norm_scale = jnp.clip(1.0 + 0.18 * jax.random.normal(arg_keys[4], (KEY_VALUE_RANK,), jnp.float32), 0.1, 1.9)
    query_plain_weight = noise(arg_keys[5], (QUERY_RANK, HEAD_COUNT * PLAIN_HEAD_SIZE), (QUERY_RANK // 6) ** -0.5, 0.375, ((1, 16),))
    query_rotary_weight = noise(arg_keys[6], (QUERY_RANK, HEAD_COUNT * ROTARY_SIZE), (QUERY_RANK // 6) ** -0.5, 0.375, ((1, 16),))
    key_up_weight = noise(arg_keys[7], (KEY_VALUE_RANK, HEAD_COUNT * PLAIN_HEAD_SIZE), KEY_VALUE_RANK ** -0.5, 0.25, ((1, 16),))
    value_up_weight = noise(arg_keys[8], (KEY_VALUE_RANK, HEAD_COUNT * VALUE_HEAD_SIZE), KEY_VALUE_RANK ** -0.5, 0.25, ((1, 16),))
    output_weight = noise(arg_keys[9], (HEAD_COUNT * VALUE_HEAD_SIZE, D), (HEAD_COUNT * VALUE_HEAD_SIZE // 16) ** -0.5, 0.75, ((1, 16),))
    mixture_input = noise(arg_keys[10], (TOKENS2, D), 1.0, 6.0, ((0, 32),))
    mixture_gain = jnp.clip(1.0 + 0.18 * jax.random.normal(arg_keys[11], (D,), jnp.float32), 0.1, 1.9)
    routes_keys = jax.random.split(jax.random.fold_in(arg_keys[12], 1), TOKENS2 // TOK2)
    routes_turns = jax.random.permutation(jax.random.fold_in(arg_keys[12], 3), TOKENS2 // TOK2)
    routes = jax.vmap(lambda own, number: assign_block(jax.random.fold_in(arg_keys[12], 2), own, number, TOK2, EXPERTS, TOPK, CAP, 1))(routes_keys, routes_turns).reshape((TOKENS2, TOPK))
    route_weight = jnp.clip(0.2 + 1.8 * jax.random.uniform(arg_keys[13], (TOKENS2, TOPK), jnp.float32) ** levels(arg_keys[13], (TOKENS2, TOPK), ((0, 32),), -0.2, 0.2), 0.2, 2.0)
    expert_gate = noise(arg_keys[14], (EXPERTS, D, EXP_FF), D ** -0.5, 0.125, ((0, 32), (2, 16)))
    expert_up = noise(arg_keys[15], (EXPERTS, D, EXP_FF), D ** -0.5, 0.125, ((0, 32), (2, 16)))
    expert_down = noise(arg_keys[16], (EXPERTS, EXP_FF, D), EXP_FF ** -0.5, 0.09375, ((0, 32), (2, 16)))
    shared_gate = noise(arg_keys[17], (D, SH_FF), D ** -0.5, 0.125, ((1, 16),))
    shared_up = noise(arg_keys[18], (D, SH_FF), D ** -0.5, 0.125, ((1, 16),))
    shared_down = noise(arg_keys[19], (SH_FF, D), SH_FF ** -0.5, 0.25, ((1, 16),))
    return dict(compressed_query=compressed_query, compressed_key_value=compressed_key_value, rotary_key=rotary_key, query_norm_scale=query_norm_scale, context_norm_scale=context_norm_scale, query_plain_weight=query_plain_weight, query_rotary_weight=query_rotary_weight, key_up_weight=key_up_weight, value_up_weight=value_up_weight, output_weight=output_weight, mixture_input=mixture_input, mixture_gain=mixture_gain, routes=routes, route_weight=route_weight, expert_gate=expert_gate, expert_up=expert_up, expert_down=expert_down, shared_gate=shared_gate, shared_up=shared_up, shared_down=shared_down)


def normed_rows(values, scaling):
    floats = values.astype(jnp.float32)
    return floats * lax.rsqrt(lax.optimization_barrier(jnp.mean(floats * floats, axis=-1, keepdims=True)) + 1e-06) * scaling

def rotary_tables(positions):
    inverse = 1.0 / 10000.0 ** (jnp.arange(0, ROTARY_SIZE, 2, dtype=jnp.float32) / ROTARY_SIZE)
    angles = positions.astype(jnp.float32)[:, None] * inverse[None, :]
    return (jnp.cos(angles), jnp.sin(angles))

def rotate(vectors, cosine, sine_part):
    half_width = vectors.shape[-1] // 2
    front_half = vectors[..., :half_width]
    back_half = vectors[..., half_width:]
    return jnp.concatenate([front_half * cosine - back_half * sine_part, front_half * sine_part + back_half * cosine], axis=-1)

def reference(compressed_query, compressed_key_value, rotary_key, query_norm_scale, context_norm_scale, query_plain_weight, query_rotary_weight, key_up_weight, value_up_weight, output_weight, mixture_input, mixture_gain, routes, route_weight, expert_gate, expert_up, expert_down, shared_gate, shared_up, shared_down):
    positions = jnp.arange(SEQUENCE_LEN1, dtype=jnp.int32)
    cosine, sine_part = rotary_tables(positions)
    compressed = normed_rows(compressed_query, query_norm_scale).astype(jnp.bfloat16)
    query_nope = jnp.dot(compressed, query_plain_weight, preferred_element_type=jnp.float32).astype(jnp.bfloat16)
    query_turn = jnp.dot(compressed, query_rotary_weight, preferred_element_type=jnp.float32).reshape(SEQUENCE_LEN1, HEAD_COUNT, ROTARY_SIZE)
    query_rot = rotate(query_turn, cosine[:, None, :], sine_part[:, None, :])
    context = normed_rows(compressed_key_value, context_norm_scale).astype(jnp.bfloat16)
    key_rot = rotate(rotary_key.astype(jnp.float32), cosine, sine_part)
    key_nope = jnp.dot(context, key_up_weight, preferred_element_type=jnp.float32).astype(jnp.bfloat16)
    value_rows = jnp.dot(context, value_up_weight, preferred_element_type=jnp.float32).astype(jnp.bfloat16)
    scale = (PLAIN_HEAD_SIZE + ROTARY_SIZE) ** (-0.5)
    rows_block = math.gcd(SEQUENCE_LEN1, 512)

    def per_head(inputs):
        head_query, head_turn, head_key, head_value = inputs

        def per_block(block_inputs):
            block_query, block_turn = block_inputs
            scores = (jnp.dot(block_query, head_key.T, preferred_element_type=jnp.float32) + jnp.dot(block_turn, key_rot.T, precision=lax.Precision.HIGHEST)) * scale
            largest = lax.optimization_barrier(jnp.max(scores, axis=-1, keepdims=True))
            weights = jnp.exp(scores - largest)
            summed = jnp.dot(weights.astype(jnp.bfloat16), head_value, preferred_element_type=jnp.float32)
            return (summed / lax.optimization_barrier(jnp.sum(weights, axis=-1, keepdims=True))).astype(jnp.bfloat16)
        blocks = lax.map(per_block, (head_query.reshape(SEQUENCE_LEN1 // rows_block, rows_block, PLAIN_HEAD_SIZE), head_turn.reshape(SEQUENCE_LEN1 // rows_block, rows_block, ROTARY_SIZE)))
        return blocks.reshape(SEQUENCE_LEN1, VALUE_HEAD_SIZE)
    heads_out = lax.map(per_head, (query_nope.reshape(SEQUENCE_LEN1, HEAD_COUNT, PLAIN_HEAD_SIZE).transpose(1, 0, 2), query_rot.transpose(1, 0, 2), key_nope.reshape(SEQUENCE_LEN1, HEAD_COUNT, PLAIN_HEAD_SIZE).transpose(1, 0, 2), value_rows.reshape(SEQUENCE_LEN1, HEAD_COUNT, VALUE_HEAD_SIZE).transpose(1, 0, 2)))
    heads_out = heads_out.transpose(1, 0, 2).reshape(SEQUENCE_LEN1, HEAD_COUNT * VALUE_HEAD_SIZE)
    attended = jnp.dot(heads_out, output_weight, preferred_element_type=jnp.float32).astype(jnp.bfloat16)
    floats = mixture_input.astype(jnp.float32)
    centred = floats - lax.optimization_barrier(jnp.mean(floats, axis=-1, keepdims=True))
    normed = (centred * lax.rsqrt(lax.optimization_barrier(jnp.mean(centred * centred, axis=-1, keepdims=True)) + 1e-05) * mixture_gain).astype(jnp.bfloat16)
    shared_hidden = (jax.nn.silu(jnp.dot(normed, shared_gate, preferred_element_type=jnp.float32)) * jnp.dot(normed, shared_up, preferred_element_type=jnp.float32)).astype(jnp.bfloat16)
    flat_routes = routes.reshape(N_EP, TOK2 * TOPK)
    one_hot = (flat_routes[:, :, None] == jnp.arange(EXPERTS, dtype=jnp.int32)[None, None, :]).astype(jnp.int32)
    ranks = lax.optimization_barrier(jnp.sum(one_hot * (jnp.cumsum(one_hot, axis=1) - 1), axis=-1))
    sources = jnp.arange(N_EP, dtype=jnp.int32)[:, None]
    place = flat_routes * (N_EP * CAP) + sources * CAP + ranks
    token_ids = sources * TOK2 + jnp.arange(TOK2 * TOPK, dtype=jnp.int32)[None, :] // TOPK
    owners = jnp.full((EXPERTS * N_EP * CAP,), TOKENS2, jnp.int32)
    owners = owners.at[place.reshape(-1)].set(token_ids.reshape(-1)).reshape(EXPERTS, N_EP * CAP)
    padded = jnp.concatenate([normed, jnp.zeros((1, D), jnp.bfloat16)], axis=0)

    def per_expert(inputs):
        owner_rows, gate_matrix, up_matrix, down_matrix = inputs
        gathered = padded[owner_rows]
        hidden = (jax.nn.silu(jnp.dot(gathered, gate_matrix, preferred_element_type=jnp.float32)) * jnp.dot(gathered, up_matrix, preferred_element_type=jnp.float32)).astype(jnp.bfloat16)
        return jnp.dot(hidden, down_matrix, preferred_element_type=jnp.float32).astype(jnp.bfloat16)
    results = lax.map(per_expert, (owners, expert_gate, expert_up, expert_down))
    picked = results.reshape(EXPERTS * N_EP * CAP, D)[place.reshape(-1)]
    picked = picked.astype(jnp.float32).reshape(TOKENS2, TOPK, D)
    routed = lax.optimization_barrier(jnp.sum(picked * route_weight[:, :, None], axis=1))
    combined = (jnp.dot(shared_hidden, shared_down, preferred_element_type=jnp.float32) + routed).astype(jnp.bfloat16)
    return (attended, combined)
```

```python
import functools

import jax
import jax.numpy as jnp
import numpy as np
from jax import lax
from jax.experimental import pallas as pl
from jax.experimental.pallas import tpu as pltpu
from jax.sharding import Mesh
from jax.sharding import PartitionSpec as P

PLAIN = 64
ROTARY = 32
VALUE = 64
EP = ("z", "core")
TP = ("y", "x")
PLANE = ("core", "y", "x")
F32 = jnp.float32
BF16 = jnp.bfloat16
VMEM = pl.BlockSpec(memory_space=pltpu.VMEM)
SMEM = pl.BlockSpec(memory_space=pltpu.SMEM)


def dot(a, b, ca=1, cb=0):
    return lax.dot_general(a, b, (((ca,), (cb,)), ((), ())), preferred_element_type=F32)


def call(body, outs, args, smem=0, flops=10**9, bytes_accessed=10**6):
    return pl.pallas_call(
        body,
        out_shape=outs,
        in_specs=[SMEM] * smem + [VMEM] * (len(args) - smem),
        out_specs=jax.tree.map(lambda _: VMEM, outs),
        cost_estimate=pl.CostEstimate(
            flops=flops, bytes_accessed=bytes_accessed, transcendentals=0
        ),
    )(*args)


def shape(dims, dtype=BF16):
    return jax.ShapeDtypeStruct(dims, dtype)


def split3(x):
    high = x.astype(BF16)
    rest = x - high.astype(F32)
    middle = rest.astype(BF16)
    low = (rest - middle.astype(F32)).astype(BF16)
    return high, middle, low


def rms(values, scaling):
    floats = values.astype(F32)
    mean = jnp.mean(floats * floats, axis=-1, keepdims=True)
    return (floats * lax.rsqrt(mean + 1e-06) * scaling).astype(BF16)


def key_value_kernel(latent, scaling, key_up, value_up, rotary, out):
    tokens = latent.shape[0]
    context = rms(latent[...], scaling[...])
    both = jnp.concatenate([dot(context, key_up[...]), dot(context, value_up[...])], axis=1)
    out[0 : PLAIN + VALUE, :] = both.T.astype(BF16)
    wide = jnp.concatenate(
        [rotary[...].astype(F32), jnp.zeros((tokens, 128 - ROTARY), F32)], axis=1
    )
    out[PLAIN + VALUE :, :] = wide.T[0:ROTARY, :].astype(BF16)


def query_kernel(place, latent, scaling, plain, rotary, cos, sin, out):
    tokens = latent.shape[0]
    compressed = rms(latent[...], scaling[...])
    wide = jnp.concatenate(
        [
            dot(compressed, plain[...]),
            dot(compressed, rotary[...]),
            jnp.zeros((tokens, 128 - PLAIN - ROTARY), F32),
        ],
        axis=1,
    ).T
    half = ROTARY // 2
    a, b = wide[PLAIN : PLAIN + half, :], wide[PLAIN + half : PLAIN + ROTARY, :]
    c, s = cos[place[0]], sin[place[0]]
    high, middle, low = split3(jnp.concatenate([a * c - b * s, a * s + b * c], axis=0))
    out[...] = jnp.concatenate(
        [wide[0:PLAIN, :].astype(BF16), high, high, middle, middle, high, low], axis=0
    )


def attention_kernel(query, kv, shared, cos, sin, out, scores):
    blocks, _, width = kv.shape
    q = query[...].astype(F32).T.astype(BF16)
    half = ROTARY // 2
    scale = (PLAIN + ROTARY) ** -0.5
    tokens = q.shape[0]

    top = jnp.full((tokens, width), -jnp.inf, F32)
    for j in range(blocks):
        raw = kv[j, PLAIN + VALUE :, :].astype(F32)
        a, b = raw[0:half, :], raw[half:, :]
        c, s = cos[j], sin[j]
        high, middle, low = split3(jnp.concatenate([a * c - b * s, a * s + b * c], axis=0))
        keys = jnp.concatenate(
            [kv[j, 0:PLAIN, :], high, middle, high, middle, low, high], axis=0
        )
        part = dot(q, keys) * scale
        scores[:, j * width : (j + 1) * width] = part
        top = jnp.maximum(top, part)
    largest = jnp.max(top, axis=1, keepdims=True)
    total = jnp.zeros((tokens, width), F32)
    summed = jnp.zeros((VALUE, tokens), F32)
    for j in range(blocks):
        weights = jnp.exp(scores[:, j * width : (j + 1) * width] - largest)
        total = total + weights
        summed = summed + dot(kv[j, PLAIN : PLAIN + VALUE, :], weights.astype(BF16), 1, 1)
    whole = jnp.broadcast_to(jnp.sum(total, axis=1, keepdims=True), (tokens, width)).T
    heads = (summed / whole[0:VALUE, :]).astype(BF16)
    sent = jnp.concatenate([heads, shared[...]], axis=0)
    for t in range(out.shape[0]):
        out[t] = sent


def dispatch_kernel(place, rows, gain, routes, gate, up, sent, slots, shared, normed, *, experts, capacity):
    tokens = rows.shape[0]
    floats = rows[...].astype(F32)
    centred = floats - jnp.mean(floats, axis=-1, keepdims=True)
    variance = jnp.mean(centred * centred, axis=-1, keepdims=True)
    values = (centred * lax.rsqrt(variance + 1e-05) * gain[...]).astype(BF16)
    normed[...] = values
    lanes = lax.broadcasted_iota(jnp.int32, (tokens, 128), 1)
    chosen = [routes[:, k : k + 1] for k in range(routes.shape[1])]
    marks = [(lanes == c) for c in chosen]
    named = sum(jnp.where(m, 1.0, 0.0) for m in marks).astype(BF16)
    earlier = (
        lax.broadcasted_iota(jnp.int32, (tokens, tokens), 0)
        > lax.broadcasted_iota(jnp.int32, (tokens, tokens), 1)
    )
    before = dot(jnp.where(earlier, 1.0, 0.0).astype(BF16), named)
    places = lax.broadcasted_iota(jnp.int32, (tokens, experts * capacity), 1)
    hot = jnp.zeros((tokens, experts * capacity), F32)
    for k, (c, m) in enumerate(zip(chosen, marks)):
        rank = jnp.sum(jnp.where(m, before, 0.0), axis=1, keepdims=True).astype(jnp.int32)
        slot = c * capacity + rank
        slots[:, k : k + 1] = slot
        hot = jnp.where(places == slot, 1.0, hot)
    width = sent.shape[1]
    own = normed[:, pl.ds(pl.multiple_of(place[1] * width, width), width)]
    sent[...] = dot(hot.T.astype(BF16), own).astype(BF16)
    g = dot(values, gate[...])
    u = dot(values, up[...])
    hidden = g / (1.0 + jnp.exp(-g)) * u
    wide = jnp.concatenate(
        [hidden, jnp.zeros((tokens, 128 - hidden.shape[1]), F32)], axis=1
    )
    shared[...] = wide.T[0 : hidden.shape[1], :].astype(BF16)


def spread_kernel(order, rows, out):
    placed = dot(order[...], rows[...]).astype(BF16)
    half = out.shape[2]
    for c in range(out.shape[0]):
        part = placed[c * half : (c + 1) * half, :]
        for t in range(out.shape[1]):
            out[c, t] = part


def expert_kernel(rows, gate, up, down, out):
    parts, wide = rows.shape[0], rows.shape[1]
    width = out.shape[3]
    for c in range(parts):
        x = jnp.concatenate([rows[c, t] for t in range(wide)], axis=1)
        g = dot(x, gate[...])
        u = dot(x, up[...])
        hidden = (g / (1.0 + jnp.exp(-g)) * u).astype(BF16)
        for t in range(wide):
            out[c, t] = dot(hidden, down[t]).astype(BF16)


def gathered_sum_kernel(order, partial, out):
    parts, wide = partial.shape[0], partial.shape[1]
    sums = []
    for c in range(parts):
        total = partial[c, 0].astype(F32)
        for t in range(1, wide):
            total = total + partial[c, t].astype(F32)
        sums.append(total.astype(BF16))
    out[...] = dot(order[...], jnp.concatenate(sums, axis=0), 0, 0).astype(BF16)


def final_kernel(returned, slots, route_weight, both, output_weight, shared_down, attended, combined):
    tokens = slots.shape[0]
    places = lax.broadcasted_iota(jnp.int32, (tokens, returned.shape[0]), 1)
    routed = jnp.zeros((tokens, returned.shape[1]), F32)
    for k in range(slots.shape[1]):
        hot = jnp.where(places == slots[:, k : k + 1], 1.0, 0.0).astype(BF16)
        routed = routed + dot(hot, returned[...]) * route_weight[:, k : k + 1]
    heads = jnp.concatenate([both[t, 0:VALUE, :] for t in range(both.shape[0])], axis=0)
    hidden = jnp.concatenate([both[t, VALUE:, :] for t in range(both.shape[0])], axis=0)
    attended[...] = dot(heads, output_weight[...], 0, 0).astype(BF16)
    combined[...] = (dot(hidden, shared_down[...], 0, 0) + routed).astype(BF16)


def tables(positions, width):
    inverse = (1.0 / 10000.0 ** (np.arange(0, ROTARY, 2) / ROTARY)).astype(np.float32)
    angles = inverse[:, None] * np.arange(positions, dtype=np.float32)[None, :]
    angles = angles.astype(np.float64).reshape(ROTARY // 2, positions // width, width)
    angles = angles.transpose(1, 0, 2)
    return np.cos(angles).astype(np.float32), np.sin(angles).astype(np.float32)


def row_order(outer, inner, capacity):
    source = np.arange(outer * inner * capacity).reshape(outer, inner, capacity)
    source = source.transpose(1, 0, 2).reshape(-1)
    return np.eye(source.size, dtype=np.float32)[source]


def exchange(array, axes):
    return lax.all_to_all(array, axes, 0, 0, tiled=True)


def per_device(
    compressed_query,
    compressed_key_value,
    rotary_key,
    query_norm_scale,
    context_norm_scale,
    query_plain_weight,
    query_rotary_weight,
    key_up_weight,
    value_up_weight,
    output_weight,
    mixture_input,
    mixture_gain,
    routes,
    route_weight,
    expert_gate,
    expert_up,
    expert_down,
    shared_gate,
    shared_up,
    shared_down,
):
    tokens, model = mixture_input.shape
    planes, cores = lax.axis_size("z"), lax.axis_size("core")
    wide = lax.axis_size(TP)
    experts = planes * cores
    width = model // wide
    capacity = tokens * routes.shape[1] * 3 // (2 * experts)
    units = expert_gate.shape[2]
    shared_units = shared_gate.shape[1]
    place = jnp.stack([lax.axis_index(EP), lax.axis_index(TP)]).astype(jnp.int32)
    cos, sin = tables(tokens * experts, tokens)
    order = jnp.asarray(row_order(planes, cores, capacity), BF16)

    down = exchange(expert_down[0].reshape(wide, units, width), TP)

    kv = call(
        key_value_kernel,
        shape((PLAIN + VALUE + ROTARY, tokens)),
        (compressed_key_value, context_norm_scale[None], key_up_weight, value_up_weight, rotary_key),
    )
    all_kv = lax.all_gather(kv, EP, axis=0, tiled=True).reshape(experts, *kv.shape)

    sent, slots, shared, _ = call(
        functools.partial(dispatch_kernel, experts=experts, capacity=capacity),
        (
            shape((experts * capacity, width)),
            shape((tokens, routes.shape[1]), jnp.int32),
            shape((shared_units, tokens)),
            shape((tokens, model)),
        ),
        (place, mixture_input, mixture_gain[None], routes, shared_gate, shared_up),
        smem=1,
    )
    query = call(
        query_kernel,
        shape((PLAIN + 6 * ROTARY, tokens)),
        (
            place,
            compressed_query,
            query_norm_scale[None],
            query_plain_weight,
            query_rotary_weight,
            cos,
            sin,
        ),
        smem=1,
    )

    moved = exchange(sent.reshape(planes, cores * capacity, width), "z")
    rows = planes * capacity
    spread = call(
        spread_kernel,
        shape((cores, wide, rows, width)),
        (order, moved.reshape(experts * capacity, width)),
    )
    arrived = exchange(spread.reshape(cores * wide, rows, width), PLANE)
    partial = call(
        expert_kernel,
        shape((cores, wide, rows, width)),
        (arrived.reshape(cores, wide, rows, width), expert_gate[0], expert_up[0], down),
    )
    parts = exchange(partial.reshape(cores * wide, rows, width), PLANE)
    summed = call(
        gathered_sum_kernel,
        shape((experts * capacity, width)),
        (order, parts.reshape(cores, wide, rows, width)),
    )
    returned = exchange(summed.reshape(planes, cores * capacity, width), "z")

    both = pl.pallas_call(
        attention_kernel,
        out_shape=shape((wide, VALUE + shared_units, tokens)),
        in_specs=[VMEM] * 5,
        out_specs=VMEM,
        scratch_shapes=[pltpu.VMEM((tokens, tokens * experts), F32)],
        cost_estimate=pl.CostEstimate(flops=10**9, bytes_accessed=10**6, transcendentals=0),
    )(query, all_kv, shared, cos, sin)
    both = exchange(both, TP)
    return call(
        final_kernel,
        (shape((tokens, width)), shape((tokens, width))),
        (
            returned.reshape(experts * capacity, width),
            slots,
            route_weight,
            both,
            output_weight,
            shared_down,
        ),
    )


def solution(mesh):
    split = Mesh(mesh.devices.reshape(16, 2, 4, 4), ("z", "core", "y", "x"))
    placed = (
        P(EP, None),
        P(EP, None),
        P(EP, None),
        P(),
        P(),
        P(None, TP),
        P(None, TP),
        P(None, TP),
        P(None, TP),
        P(None, TP),
        P(EP, None),
        P(),
        P(EP, None),
        P(EP, None),
        P(EP, None, TP),
        P(EP, None, TP),
        P(EP, None, TP),
        P(None, TP),
        P(None, TP),
        P(None, TP),
    )
    return jax.shard_map(
        per_device,
        mesh=split,
        in_specs=placed,
        out_specs=(P(EP, TP), P(EP, TP)),
        check_vma=False,
    )
```

```python
import functools

import jax
import jax.numpy as jnp
import numpy as np
from jax import lax
from jax.experimental import pallas as pl
from jax.experimental.pallas import tpu as pltpu
from jax.sharding import Mesh
from jax.sharding import PartitionSpec as P

PLAIN = 64
ROTARY = 32
VALUE = 64
EP = ("z", "core")
TP = ("y", "x")
PLANE = ("core", "y", "x")
F32 = jnp.float32
BF16 = jnp.bfloat16
VMEM = pl.BlockSpec(memory_space=pltpu.VMEM)
SMEM = pl.BlockSpec(memory_space=pltpu.SMEM)


def dot(a, b, ca=1, cb=0):
    return lax.dot_general(a, b, (((ca,), (cb,)), ((), ())), preferred_element_type=F32)


def call(body, outs, args, smem=0, scratch=(), limit=8):
    return pl.pallas_call(
        body,
        out_shape=outs,
        in_specs=[SMEM] * smem + [VMEM] * (len(args) - smem),
        out_specs=jax.tree.map(lambda _: VMEM, outs),
        scratch_shapes=scratch,
        compiler_params=pltpu.CompilerParams(vmem_limit_bytes=limit << 20),
        cost_estimate=pl.CostEstimate(flops=10**9, bytes_accessed=10**6, transcendentals=0),
    )(*args)


def shape(dims, dtype=BF16):
    return jax.ShapeDtypeStruct(dims, dtype)


def split3(x):
    high = x.astype(BF16)
    rest = x - high.astype(F32)
    middle = rest.astype(BF16)
    low = (rest - middle.astype(F32)).astype(BF16)
    return high, middle, low


def rms(values, scaling):
    floats = values.astype(F32)
    mean = jnp.mean(floats * floats, axis=-1, keepdims=True)
    return (floats * lax.rsqrt(mean + 1e-06) * scaling).astype(BF16)


def key_value_kernel(latent, scaling, key_up, value_up, rotary, out):
    context = rms(latent[...], scaling[...])
    out[0:PLAIN, :] = dot(key_up[...], context, 1, 1).astype(BF16)
    out[PLAIN : PLAIN + VALUE, :] = dot(value_up[...], context, 1, 1).astype(BF16)
    out[PLAIN + VALUE :, :] = rotary[...]


def query_kernel(place, latent, scaling, plain, rotary, cos, sin, out):
    compressed = rms(latent[...], scaling[...])
    nope = dot(plain[...], compressed, 1, 1).astype(BF16)
    turn = dot(rotary[...], compressed, 1, 1)
    half = ROTARY // 2
    a, b = turn[0:half, :], turn[half:, :]
    c, s = cos[place[0]], sin[place[0]]
    high, middle, low = split3(jnp.concatenate([a * c - b * s, a * s + b * c], axis=0))
    whole = jnp.concatenate([nope, high, high, middle, middle, high, low], axis=0)
    out[...] = whole.astype(F32).T.astype(BF16)


def attention_kernel(place, query, mine, other, shared, cos, sin, out, scores, *, order):
    q = query[...]
    planes, _, width = mine.shape
    half = ROTARY // 2
    scale = (PLAIN + ROTARY) ** -0.5
    tokens = q.shape[0]
    blocks = [(kv, j) for kv in (mine, other) for j in range(planes)]

    top = jnp.full((tokens, width), -jnp.inf, F32)
    for n, (kv, j) in enumerate(blocks):
        core = place[2] if kv is mine else 1 - place[2]
        at = ((place[1] + (planes - order[j])) % planes) * 2 + core
        raw = kv[j, PLAIN + VALUE :, :].astype(F32)
        a, b = raw[0:half, :], raw[half:, :]
        c, s = cos[at], sin[at]
        high, middle, low = split3(jnp.concatenate([a * c - b * s, a * s + b * c], axis=0))
        keys = jnp.concatenate(
            [kv[j, 0:PLAIN, :], high, middle, high, middle, low, high], axis=0
        )
        part = dot(q, keys) * scale
        scores[:, n * width : (n + 1) * width] = part
        top = jnp.maximum(top, part)
    largest = jnp.max(top, axis=1, keepdims=True)
    total = jnp.zeros((tokens, width), F32)
    summed = jnp.zeros((VALUE, tokens), F32)
    for n, (kv, j) in enumerate(blocks):
        weights = jnp.exp(scores[:, n * width : (n + 1) * width] - largest)
        total = total + weights
        summed = summed + dot(kv[j, PLAIN : PLAIN + VALUE, :], weights.astype(BF16), 1, 1)
    whole = jnp.broadcast_to(jnp.sum(total, axis=1, keepdims=True), (tokens, width)).T
    heads = (summed / whole[0:VALUE, :]).astype(BF16)
    sent = jnp.concatenate([heads, shared[...]], axis=0)
    for t in range(out.shape[0]):
        out[t] = sent


def one_hot(slots, k, rows):
    places = lax.broadcasted_iota(jnp.int32, (rows, slots.shape[1]), 0)
    return jnp.where(places == slots[k : k + 1, :], 1.0, 0.0)


def dispatch_kernel(place, rows, gain, routes, gate, up, sent, slots, shared, normed, *, experts, capacity):
    tokens = rows.shape[0]
    floats = rows[...].astype(F32)
    centred = floats - jnp.mean(floats, axis=-1, keepdims=True)
    variance = jnp.mean(centred * centred, axis=-1, keepdims=True)
    values = (centred * lax.rsqrt(variance + 1e-05) * gain[...]).astype(BF16)
    normed[...] = values
    marks = [one_hot(routes, k, experts) for k in range(routes.shape[0])]
    earlier = (
        lax.broadcasted_iota(jnp.int32, (tokens, tokens), 0)
        < lax.broadcasted_iota(jnp.int32, (tokens, tokens), 1)
    )
    before = dot(sum(marks).astype(BF16), jnp.where(earlier, 1.0, 0.0).astype(BF16))
    for k, mark in enumerate(marks):
        rank = jnp.sum(mark * before, axis=0, keepdims=True).astype(jnp.int32)
        slots[k : k + 1, :] = routes[k : k + 1, :] * capacity + rank
    hot = one_hot(slots, 0, experts * capacity)
    for k in range(1, routes.shape[0]):
        hot = hot + one_hot(slots, k, experts * capacity)
    width = sent.shape[1]
    own = normed[:, pl.ds(pl.multiple_of(place[3] * width, width), width)]
    sent[...] = dot(hot.astype(BF16), own).astype(BF16)
    g = dot(gate[...], values, 1, 1)
    u = dot(up[...], values, 1, 1)
    shared[...] = (g / (1.0 + jnp.exp(-g)) * u).astype(BF16)


def spread_kernel(order, rows, out):
    placed = dot(order[...], rows[...]).astype(BF16)
    half = out.shape[2]
    for c in range(out.shape[0]):
        part = placed[c * half : (c + 1) * half, :]
        for t in range(out.shape[1]):
            out[c, t] = part


def expert_kernel(rows, gate, up, down, out):
    parts, wide = rows.shape[0], rows.shape[1]
    for c in range(parts):
        x = jnp.concatenate([rows[c, t] for t in range(wide)], axis=1)
        g = dot(x, gate[...])
        u = dot(x, up[...])
        hidden = (g / (1.0 + jnp.exp(-g)) * u).astype(BF16)
        for t in range(wide):
            out[c, t] = dot(hidden, down[t]).astype(BF16)


def gathered_sum_kernel(order, partial, out):
    parts, wide = partial.shape[0], partial.shape[1]
    sums = []
    for c in range(parts):
        total = partial[c, 0].astype(F32)
        for t in range(1, wide):
            total = total + partial[c, t].astype(F32)
        sums.append(total.astype(BF16))
    out[...] = dot(order[...], jnp.concatenate(sums, axis=0), 0, 0).astype(BF16)


def final_kernel(returned, slots, route_weight, both, output_weight, shared_down, attended, combined):
    tokens, width = slots.shape[1], returned.shape[1]
    routed = jnp.zeros((tokens, width), F32)
    for k in range(slots.shape[0]):
        hot = one_hot(slots, k, returned.shape[0]).astype(BF16)
        scale = jnp.broadcast_to(route_weight[k : k + 1, :], (width, tokens)).T
        routed = routed + dot(hot, returned[...], 0, 0) * scale
    heads = jnp.concatenate([both[t, 0:VALUE, :] for t in range(both.shape[0])], axis=0)
    hidden = jnp.concatenate([both[t, VALUE:, :] for t in range(both.shape[0])], axis=0)
    attended[...] = dot(heads, output_weight[...], 0, 0).astype(BF16)
    combined[...] = (dot(hidden, shared_down[...], 0, 0) + routed).astype(BF16)


def tables(positions, width):
    inverse = (1.0 / 10000.0 ** (np.arange(0, ROTARY, 2) / ROTARY)).astype(np.float32)
    angles = inverse[:, None] * np.arange(positions, dtype=np.float32)[None, :]
    angles = angles.astype(np.float64).reshape(ROTARY // 2, positions // width, width)
    angles = angles.transpose(1, 0, 2)
    return np.cos(angles).astype(np.float32), np.sin(angles).astype(np.float32)


def row_order(outer, inner, capacity):
    source = np.arange(outer * inner * capacity).reshape(outer, inner, capacity)
    source = source.transpose(1, 0, 2).reshape(-1)
    return np.eye(source.size, dtype=np.float32)[source]


def exchange(array, axes):
    return lax.all_to_all(array, axes, 0, 0, tiled=True)


def per_device(
    compressed_query,
    compressed_key_value,
    rotary_key,
    query_norm_scale,
    context_norm_scale,
    query_plain_weight,
    query_rotary_weight,
    key_up_weight,
    value_up_weight,
    output_weight,
    mixture_input,
    mixture_gain,
    routes,
    route_weight,
    expert_gate,
    expert_up,
    expert_down,
    shared_gate,
    shared_up,
    shared_down,
):
    tokens, model = mixture_input.shape
    planes, cores = lax.axis_size("z"), lax.axis_size("core")
    wide = lax.axis_size(TP)
    experts = planes * cores
    width = model // wide
    capacity = tokens * routes.shape[1] * 3 // (2 * experts)
    units = expert_gate.shape[2]
    shared_units = shared_gate.shape[1]
    place = jnp.stack(
        [lax.axis_index(EP), lax.axis_index("z"), lax.axis_index("core"), lax.axis_index(TP)]
    ).astype(jnp.int32)
    cos, sin = tables(tokens * experts, tokens)
    order = jnp.asarray(row_order(planes, cores, capacity), BF16)

    down = exchange(expert_down[0].reshape(wide, units, width), TP)

    kv = call(
        key_value_kernel,
        shape((PLAIN + VALUE + ROTARY, tokens)),
        (
            compressed_key_value,
            context_norm_scale[None],
            key_up_weight.T,
            value_up_weight.T,
            rotary_key.T,
        ),
    )
    mine, behind, step = kv[None], [0], planes // 2
    while step:
        ring = [(z, (z + step) % planes) for z in range(planes)]
        received = lax.ppermute(mine, "z", ring)
        mine = jnp.concatenate([mine, received], axis=0)
        behind = behind + [(b + step) % planes for b in behind]
        step //= 2
    other = lax.ppermute(mine, "core", [(0, 1), (1, 0)])

    sent, slots, shared, _ = call(
        functools.partial(dispatch_kernel, experts=experts, capacity=capacity),
        (
            shape((experts * capacity, width)),
            shape((routes.shape[1], tokens), jnp.int32),
            shape((shared_units, tokens)),
            shape((tokens, model)),
        ),
        (place, mixture_input, mixture_gain[None], routes.T, shared_gate.T, shared_up.T),
        smem=1,
        limit=12,
    )
    query = call(
        query_kernel,
        shape((tokens, PLAIN + 6 * ROTARY)),
        (
            place,
            compressed_query,
            query_norm_scale[None],
            query_plain_weight.T,
            query_rotary_weight.T,
            cos,
            sin,
        ),
        smem=1,
    )

    moved = exchange(sent.reshape(planes, cores * capacity, width), "z")
    rows = planes * capacity
    spread = call(
        spread_kernel,
        shape((cores, wide, rows, width)),
        (order, moved.reshape(experts * capacity, width)),
    )
    arrived = exchange(spread.reshape(cores * wide, rows, width), PLANE)
    partial = call(
        expert_kernel,
        shape((cores, wide, rows, width)),
        (arrived.reshape(cores, wide, rows, width), expert_gate[0], expert_up[0], down),
        limit=16,
    )
    parts = exchange(partial.reshape(cores * wide, rows, width), PLANE)
    summed = call(
        gathered_sum_kernel,
        shape((experts * capacity, width)),
        (order, parts.reshape(cores, wide, rows, width)),
    )
    returned = exchange(summed.reshape(planes, cores * capacity, width), "z")

    both = call(
        functools.partial(attention_kernel, order=behind),
        shape((wide, VALUE + shared_units, tokens)),
        (place, query, mine, other, shared, cos, sin),
        smem=1,
        scratch=[pltpu.VMEM((tokens, tokens * experts), F32)],
        limit=12,
    )
    both = exchange(both, TP)
    return call(
        final_kernel,
        (shape((tokens, width)), shape((tokens, width))),
        (
            returned.reshape(experts * capacity, width),
            slots,
            route_weight.T,
            both,
            output_weight,
            shared_down,
        ),
    )


def solution(mesh):
    split = Mesh(mesh.devices.reshape(16, 2, 4, 4), ("z", "core", "y", "x"))
    placed = (
        P(EP, None),
        P(EP, None),
        P(EP, None),
        P(),
        P(),
        P(None, TP),
        P(None, TP),
        P(None, TP),
        P(None, TP),
        P(None, TP),
        P(EP, None),
        P(),
        P(EP, None),
        P(EP, None),
        P(EP, None, TP),
        P(EP, None, TP),
        P(EP, None, TP),
        P(None, TP),
        P(None, TP),
        P(None, TP),
    )

    return jax.shard_map(
        per_device,
        mesh=split,
        in_specs=placed,
        out_specs=(P(EP, TP), P(EP, TP)),
        check_vma=False,
    )
```

```python
import functools

import jax
import jax.numpy as jnp
import numpy as np
from jax import lax
from jax.experimental import pallas as pl
from jax.experimental.pallas import tpu as pltpu
from jax.sharding import Mesh
from jax.sharding import PartitionSpec as P

PLAIN = 64
ROTARY = 32
VALUE = 64
EP = ("z", "core")
TP = ("y", "x")
F32 = jnp.float32
BF16 = jnp.bfloat16
VMEM = pl.BlockSpec(memory_space=pltpu.VMEM)
SMEM = pl.BlockSpec(memory_space=pltpu.SMEM)


def dot(a, b, ca=1, cb=0):
    return lax.dot_general(a, b, (((ca,), (cb,)), ((), ())), preferred_element_type=F32)


def call(body, outs, args, smem=0, scratch=(), limit=8):
    return pl.pallas_call(
        body,
        out_shape=outs,
        in_specs=[SMEM] * smem + [VMEM] * (len(args) - smem),
        out_specs=jax.tree.map(lambda _: VMEM, outs),
        scratch_shapes=scratch,
        compiler_params=pltpu.CompilerParams(vmem_limit_bytes=limit << 20),
        cost_estimate=pl.CostEstimate(flops=10**9, bytes_accessed=10**6, transcendentals=0),
    )(*args)


def shape(dims, dtype=BF16):
    return jax.ShapeDtypeStruct(dims, dtype)


def split3(x):
    high = x.astype(BF16)
    rest = x - high.astype(F32)
    middle = rest.astype(BF16)
    low = (rest - middle.astype(F32)).astype(BF16)
    return high, middle, low


def rms(values, scaling):
    floats = values.astype(F32)
    mean = jnp.mean(floats * floats, axis=-1, keepdims=True)
    return (floats * lax.rsqrt(mean + 1e-06) * scaling).astype(BF16)


def key_value_kernel(latent, scaling, key_up, value_up, rotary, out):
    context = rms(latent[...], scaling[...])
    out[0:PLAIN, :] = dot(key_up[...], context, 1, 1).astype(BF16)
    out[PLAIN : PLAIN + VALUE, :] = dot(value_up[...], context, 1, 1).astype(BF16)
    out[PLAIN + VALUE :, :] = rotary[...]


def query_kernel(place, latent, scaling, plain, rotary, cos, sin, out):
    compressed = rms(latent[...], scaling[...])
    nope = dot(plain[...], compressed, 1, 1).astype(BF16)
    turn = dot(rotary[...], compressed, 1, 1)
    half = ROTARY // 2
    a, b = turn[0:half, :], turn[half:, :]
    c, s = cos[place[0]], sin[place[0]]
    high, middle, low = split3(jnp.concatenate([a * c - b * s, a * s + b * c], axis=0))
    whole = jnp.concatenate([nope, high, high, middle, middle, high, low], axis=0)
    out[...] = whole.astype(F32).T.astype(BF16)


def attention_kernel(query, kv, shared, cos, sin, out, scores):
    q = query[...]
    blocks, _, width = kv.shape
    half = ROTARY // 2
    scale = (PLAIN + ROTARY) ** -0.5
    tokens = q.shape[0]

    top = jnp.full((tokens, width), -jnp.inf, F32)
    for j in range(blocks):
        raw = kv[j, PLAIN + VALUE :, :].astype(F32)
        a, b = raw[0:half, :], raw[half:, :]
        c, s = cos[j], sin[j]
        high, middle, low = split3(jnp.concatenate([a * c - b * s, a * s + b * c], axis=0))
        keys = jnp.concatenate(
            [kv[j, 0:PLAIN, :], high, middle, high, middle, low, high], axis=0
        )
        part = dot(q, keys) * scale
        scores[:, j * width : (j + 1) * width] = part
        top = jnp.maximum(top, part)
    largest = jnp.max(top, axis=1, keepdims=True)
    total = jnp.zeros((tokens, width), F32)
    summed = jnp.zeros((VALUE, tokens), F32)
    for j in range(blocks):
        weights = jnp.exp(scores[:, j * width : (j + 1) * width] - largest)
        total = total + weights
        summed = summed + dot(kv[j, PLAIN : PLAIN + VALUE, :], weights.astype(BF16), 1, 1)
    whole = jnp.broadcast_to(jnp.sum(total, axis=1, keepdims=True), (tokens, width)).T
    heads = (summed / whole[0:VALUE, :]).astype(BF16)
    out[0] = jnp.concatenate([heads, shared[...]], axis=0)


def one_hot(slots, k, rows):
    places = lax.broadcasted_iota(jnp.int32, (rows, slots.shape[1]), 0)
    return jnp.where(places == slots[k : k + 1, :], 1.0, 0.0)


def dispatch_kernel(place, rows, gain, routes, gate, up, sent, slots, shared, normed, *, experts, capacity):
    tokens = rows.shape[0]
    floats = rows[...].astype(F32)
    centred = floats - jnp.mean(floats, axis=-1, keepdims=True)
    variance = jnp.mean(centred * centred, axis=-1, keepdims=True)
    values = (centred * lax.rsqrt(variance + 1e-05) * gain[...]).astype(BF16)
    normed[...] = values
    marks = [one_hot(routes, k, experts) for k in range(routes.shape[0])]
    earlier = (
        lax.broadcasted_iota(jnp.int32, (tokens, tokens), 0)
        < lax.broadcasted_iota(jnp.int32, (tokens, tokens), 1)
    )
    before = dot(sum(marks).astype(BF16), jnp.where(earlier, 1.0, 0.0).astype(BF16))
    for k, mark in enumerate(marks):
        rank = jnp.sum(mark * before, axis=0, keepdims=True).astype(jnp.int32)
        slots[k : k + 1, :] = routes[k : k + 1, :] * capacity + rank
    hot = one_hot(slots, 0, experts * capacity)
    for k in range(1, routes.shape[0]):
        hot = hot + one_hot(slots, k, experts * capacity)
    width = sent.shape[1]
    own = normed[:, pl.ds(pl.multiple_of(place[3] * width, width), width)]
    sent[...] = dot(hot.astype(BF16), own).astype(BF16)
    g = dot(gate[...], values, 1, 1)
    u = dot(up[...], values, 1, 1)
    shared[...] = (g / (1.0 + jnp.exp(-g)) * u).astype(BF16)


def order_kernel(order, rows, out):
    out[...] = dot(order[...], rows[...]).astype(BF16)


def spread_kernel(rows, out):
    for t in range(out.shape[0]):
        out[t] = rows[...]


def hidden_kernel(rows, gate, up, out, *, parts):
    wide, length = rows.shape[0], rows.shape[1] // parts
    for c in range(parts):
        part = slice(c * length, (c + 1) * length)
        x = jnp.concatenate([rows[t, part, :] for t in range(wide)], axis=1)
        g = dot(x, gate[...])
        u = dot(x, up[...])
        hidden = (g / (1.0 + jnp.exp(-g)) * u).astype(BF16)
        for t in range(out.shape[0]):
            out[t, part, :] = hidden


def down_kernel(place, hidden, *rest):
    downs, out = rest[:-1], rest[-1]
    parts, tall, length = out.shape[0], out.shape[1], out.shape[2]
    x = jnp.concatenate([hidden[t] for t in range(hidden.shape[0])], axis=1)
    for k, down in enumerate(downs):
        to = (place[4] + (tall - k)) % tall
        result = dot(x, down[...]).astype(BF16)
        for c in range(parts):
            out[c, to] = result[c * length : (c + 1) * length, :]


def gathered_sum_kernel(order, partial, out):
    parts, wide = partial.shape[0], partial.shape[1]
    sums = []
    for c in range(parts):
        total = partial[c, 0].astype(F32)
        for t in range(1, wide):
            total = total + partial[c, t].astype(F32)
        sums.append(total.astype(BF16))
    out[...] = dot(order[...], jnp.concatenate(sums, axis=0), 0, 0).astype(BF16)


def final_kernel(place, returned, slots, route_weight, output_weight, shared_down, *rest):
    both, (attended, combined) = rest[:-2], rest[-2:]
    tokens, width = slots.shape[1], returned.shape[1]
    routed = jnp.zeros((tokens, width), F32)
    for k in range(slots.shape[0]):
        hot = one_hot(slots, k, returned.shape[0]).astype(BF16)
        scale = jnp.broadcast_to(route_weight[k : k + 1, :], (width, tokens)).T
        routed = routed + dot(hot, returned[...], 0, 0) * scale
    tall, across = len(both), both[0].shape[0]
    units = both[0].shape[1] - VALUE
    heads, hidden, heads_weight, hidden_weight = [], [], [], []
    for a in range(tall):
        for b in range(across):
            at = (place[4] + (tall - a)) % tall * across + (place[5] + (across - b)) % across
            heads.append(both[a][b, 0:VALUE, :])
            hidden.append(both[a][b, VALUE:, :])
            heads_weight.append(output_weight[pl.ds(pl.multiple_of(at * VALUE, VALUE), VALUE), :])
            hidden_weight.append(shared_down[pl.ds(pl.multiple_of(at * units, units), units), :])
    joined = [jnp.concatenate(p, axis=0) for p in (heads, heads_weight, hidden, hidden_weight)]
    attended[...] = dot(joined[0], joined[1], 0, 0).astype(BF16)
    combined[...] = (dot(joined[2], joined[3], 0, 0) + routed).astype(BF16)


def tables(positions, width):
    inverse = (1.0 / 10000.0 ** (np.arange(0, ROTARY, 2) / ROTARY)).astype(np.float32)
    angles = inverse[:, None] * np.arange(positions, dtype=np.float32)[None, :]
    angles = angles.astype(np.float64).reshape(ROTARY // 2, positions // width, width)
    angles = angles.transpose(1, 0, 2)
    return np.cos(angles).astype(np.float32), np.sin(angles).astype(np.float32)


def row_order(outer, inner, capacity):
    source = np.arange(outer * inner * capacity).reshape(outer, inner, capacity)
    source = source.transpose(1, 0, 2).reshape(-1)
    return np.eye(source.size, dtype=np.float32)[source]


def exchange(array, axes):
    return lax.all_to_all(array, axes, 0, 0, tiled=True)


def per_device(
    compressed_query,
    compressed_key_value,
    rotary_key,
    query_norm_scale,
    context_norm_scale,
    query_plain_weight,
    query_rotary_weight,
    key_up_weight,
    value_up_weight,
    output_weight,
    mixture_input,
    mixture_gain,
    routes,
    route_weight,
    expert_gate,
    expert_up,
    expert_down,
    shared_gate,
    shared_up,
    shared_down,
):
    tokens, model = mixture_input.shape
    planes, cores = lax.axis_size("z"), lax.axis_size("core")
    wide = lax.axis_size(TP)
    experts = planes * cores
    width = model // wide
    capacity = tokens * routes.shape[1] * 3 // (2 * experts)
    units = expert_gate.shape[2]
    shared_units = shared_gate.shape[1]
    tall, across = lax.axis_size("y"), lax.axis_size("x")
    row = lax.axis_index("y")
    place = jnp.stack(
        [
            lax.axis_index(EP),
            lax.axis_index("z"),
            lax.axis_index("core"),
            lax.axis_index(TP),
            row,
            lax.axis_index("x"),
        ]
    ).astype(jnp.int32)
    cos, sin = tables(tokens * experts, tokens)
    order = jnp.asarray(row_order(planes, cores, capacity), BF16)

    kv = call(
        key_value_kernel,
        shape((PLAIN + VALUE + ROTARY, tokens)),
        (
            compressed_key_value,
            context_norm_scale[None],
            key_up_weight.T,
            value_up_weight.T,
            rotary_key.T,
        ),
        limit=56,
    )
    all_kv = lax.all_gather(kv, EP, axis=0, tiled=True).reshape(experts, *kv.shape)

    band = across * units
    downs = []
    for k in range(tall):
        part = lax.dynamic_slice_in_dim(expert_down[0], (row + k) % tall * band, band, 0)
        if k:
            part = lax.ppermute(part, "y", [(y, (y + k) % tall) for y in range(tall)])
        downs.append(part)

    sent, slots, shared, _ = call(
        functools.partial(dispatch_kernel, experts=experts, capacity=capacity),
        (
            shape((experts * capacity, width)),
            shape((routes.shape[1], tokens), jnp.int32),
            shape((shared_units, tokens)),
            shape((tokens, model)),
        ),
        (place, mixture_input, mixture_gain[None], routes.T, shared_gate.T, shared_up.T),
        smem=1,
        limit=12,
    )
    query = call(
        query_kernel,
        shape((tokens, PLAIN + 6 * ROTARY)),
        (
            place,
            compressed_query,
            query_norm_scale[None],
            query_plain_weight.T,
            query_rotary_weight.T,
            cos,
            sin,
        ),
        smem=1,
    )

    moved = exchange(sent.reshape(planes, cores * capacity, width), "z")
    rows = planes * capacity
    moved = call(
        order_kernel,
        shape((experts * capacity, width)),
        (order, moved.reshape(experts * capacity, width)),
    )
    moved = exchange(moved.reshape(cores, rows, width), "core")
    spread = call(
        spread_kernel,
        shape((wide, cores * rows, width)),
        (moved.reshape(cores * rows, width),),
    )
    arrived = exchange(spread, TP)
    hidden = call(
        functools.partial(hidden_kernel, parts=cores),
        shape((across, cores * rows, units)),
        (arrived, expert_gate[0], expert_up[0]),
        limit=14,
    )
    hidden = exchange(hidden, "x")
    partial = call(
        down_kernel,
        shape((cores, tall, rows, width)),
        (place, hidden, *downs),
        smem=1,
        limit=10,
    )
    parts = exchange(partial.reshape(cores * tall, rows, width), ("core", "y"))
    summed = call(
        gathered_sum_kernel,
        shape((experts * capacity, width)),
        (order, parts.reshape(cores, tall, rows, width)),
    )
    returned = exchange(summed.reshape(planes, cores * capacity, width), "z")

    both = call(
        attention_kernel,
        shape((1, VALUE + shared_units, tokens)),
        (query, all_kv, shared, cos, sin),
        scratch=[pltpu.VMEM((tokens, tokens * experts), F32)],
        limit=12,
    )
    pieces = [both]
    for k in range(1, across):
        pieces.append(lax.ppermute(both, "x", [(x, (x + k) % across) for x in range(across)]))
    both = jnp.concatenate(pieces, axis=0)
    pieces = [both]
    for k in range(1, tall):
        pieces.append(lax.ppermute(both, "y", [(y, (y + k) % tall) for y in range(tall)]))
    return call(
        final_kernel,
        (shape((tokens, width)), shape((tokens, width))),
        (
            place,
            returned.reshape(experts * capacity, width),
            slots,
            route_weight.T,
            output_weight,
            shared_down,
            *pieces,
        ),
        smem=1,
    )


def solution(mesh):
    split = Mesh(mesh.devices.reshape(16, 2, 4, 4), ("z", "core", "y", "x"))
    placed = (
        P(EP, None),
        P(EP, None),
        P(EP, None),
        P(),
        P(),
        P(None, TP),
        P(None, TP),
        P(None, TP),
        P(None, TP),
        P(None, TP),
        P(EP, None),
        P(),
        P(EP, None),
        P(EP, None),
        P(EP, None, TP),
        P(EP, None, TP),
        P(EP, None, TP),
        P(None, TP),
        P(None, TP),
        P(None, TP),
    )

    return jax.shard_map(
        per_device,
        mesh=split,
        in_specs=placed,
        out_specs=(P(EP, TP), P(EP, TP)),
        check_vma=False,
    )
```

```python
import functools

import jax
import jax.numpy as jnp
import numpy as np
from jax import lax
from jax.experimental import pallas as pl
from jax.experimental.pallas import tpu as pltpu
from jax.sharding import Mesh
from jax.sharding import PartitionSpec as P

PLAIN = 64
ROTARY = 32
VALUE = 64
EP = ("z", "core")
TP = ("y", "x")
F32 = jnp.float32
BF16 = jnp.bfloat16
VMEM = pl.BlockSpec(memory_space=pltpu.VMEM)
SMEM = pl.BlockSpec(memory_space=pltpu.SMEM)


def dot(a, b, ca=1, cb=0):
    return lax.dot_general(a, b, (((ca,), (cb,)), ((), ())), preferred_element_type=F32)


def call(body, outs, args, smem=0, scratch=(), limit=8):
    return pl.pallas_call(
        body,
        out_shape=outs,
        in_specs=[SMEM] * smem + [VMEM] * (len(args) - smem),
        out_specs=jax.tree.map(lambda _: VMEM, outs),
        scratch_shapes=scratch,
        compiler_params=pltpu.CompilerParams(vmem_limit_bytes=limit << 20),
        cost_estimate=pl.CostEstimate(flops=10**9, bytes_accessed=10**6, transcendentals=0),
    )(*args)


def shape(dims, dtype=BF16):
    return jax.ShapeDtypeStruct(dims, dtype)


def split3(x):
    high = x.astype(BF16)
    rest = x - high.astype(F32)
    middle = rest.astype(BF16)
    low = (rest - middle.astype(F32)).astype(BF16)
    return high, middle, low


def rms(values, scaling):
    floats = values.astype(F32)
    mean = jnp.mean(floats * floats, axis=-1, keepdims=True)
    return (floats * lax.rsqrt(mean + 1e-06) * scaling).astype(BF16)


def key_value_kernel(latent, scaling, key_up, value_up, rotary, out):
    context = rms(latent[...], scaling[...])
    both = jnp.concatenate([key_up[...], value_up[...]], axis=0)
    out[0 : PLAIN + VALUE, :] = dot(both, context, 1, 1).astype(BF16)
    out[PLAIN + VALUE :, :] = rotary[...]


def query_kernel(place, latent, scaling, plain, rotary, cos, sin, out):
    compressed = rms(latent[...], scaling[...])
    nope = dot(plain[...], compressed, 1, 1).astype(BF16)
    turn = dot(rotary[...], compressed, 1, 1)
    half = ROTARY // 2
    a, b = turn[0:half, :], turn[half:, :]
    c, s = cos[place[0]], sin[place[0]]
    high, middle, low = split3(jnp.concatenate([a * c - b * s, a * s + b * c], axis=0))
    whole = jnp.concatenate([nope, high, high, middle, middle, high, low], axis=0)
    out[...] = whole.astype(F32).T.astype(BF16)


def attention_kernel(query, kv, shared, cos, sin, out, scores):
    blocks, _, width = kv.shape
    q = query[...]
    half = ROTARY // 2
    scale = (PLAIN + ROTARY) ** -0.5
    tokens = q.shape[0]

    def keys(j):
        raw = kv[j, PLAIN + VALUE :, :].astype(F32)
        a, b = raw[0:half, :], raw[half:, :]
        c, s = cos[j], sin[j]
        high, middle, low = split3(jnp.concatenate([a * c - b * s, a * s + b * c], axis=0))
        return jnp.concatenate(
            [kv[j, 0:PLAIN, :], high, middle, high, middle, low, high], axis=0
        )

    def place(j):
        return slice(j * width, (j + 2) * width)

    top = jnp.full((tokens, 2 * width), -jnp.inf, F32)
    for j in range(0, blocks, 2):
        part = dot(q, jnp.concatenate([keys(j), keys(j + 1)], axis=1)) * scale
        scores[:, place(j)] = part
        top = jnp.maximum(top, part)
    largest = jnp.max(top, axis=1, keepdims=True)
    total = jnp.zeros((tokens, 2 * width), F32)
    summed = jnp.zeros((VALUE, tokens), F32)
    for j in range(0, blocks, 2):
        weights = jnp.exp(scores[:, place(j)] - largest)
        total = total + weights
        values = [kv[k, PLAIN : PLAIN + VALUE, :] for k in (j, j + 1)]
        summed = summed + dot(jnp.concatenate(values, axis=1), weights.astype(BF16), 1, 1)
    whole = jnp.broadcast_to(jnp.sum(total, axis=1, keepdims=True), (tokens, tokens)).T
    heads = (summed / whole[0:VALUE, :]).astype(BF16)
    out[0] = jnp.concatenate([heads, shared[...]], axis=0)


def one_hot(slots, k, rows):
    places = lax.broadcasted_iota(jnp.int32, (rows, slots.shape[1]), 0)
    return jnp.where(places == slots[k : k + 1, :], 1.0, 0.0)


def dispatch_kernel(place, rows, gain, routes, gate, up, sent, slots, shared, normed, *, experts, capacity):
    tokens = rows.shape[0]
    floats = rows[...].astype(F32)
    centred = floats - jnp.mean(floats, axis=-1, keepdims=True)
    variance = jnp.mean(centred * centred, axis=-1, keepdims=True)
    values = (centred * lax.rsqrt(variance + 1e-05) * gain[...]).astype(BF16)
    normed[...] = values
    marks = [one_hot(routes, k, experts) for k in range(routes.shape[0])]
    earlier = (
        lax.broadcasted_iota(jnp.int32, (tokens, tokens), 0)
        < lax.broadcasted_iota(jnp.int32, (tokens, tokens), 1)
    )
    before = dot(sum(marks).astype(BF16), jnp.where(earlier, 1.0, 0.0).astype(BF16))
    for k, mark in enumerate(marks):
        rank = jnp.sum(mark * before, axis=0, keepdims=True).astype(jnp.int32)
        slots[k : k + 1, :] = routes[k : k + 1, :] * capacity + rank
    hot = one_hot(slots, 0, experts * capacity)
    for k in range(1, routes.shape[0]):
        hot = hot + one_hot(slots, k, experts * capacity)
    width = sent.shape[1]
    own = normed[:, pl.ds(pl.multiple_of(place[3] * width, width), width)]
    sent[...] = dot(hot.astype(BF16), own).astype(BF16)
    g = dot(gate[...], values, 1, 1)
    u = dot(up[...], values, 1, 1)
    shared[...] = (g / (1.0 + jnp.exp(-g)) * u).astype(BF16)


def order_kernel(order, rows, out):
    out[...] = dot(order[...], rows[...]).astype(BF16)


def spread_kernel(rows, out):
    for t in range(out.shape[0]):
        out[t] = rows[...]


def hidden_kernel(rows, gate, up, out, *, parts):
    wide, length = rows.shape[0], rows.shape[1] // parts
    for c in range(parts):
        part = slice(c * length, (c + 1) * length)
        x = jnp.concatenate([rows[t, part, :] for t in range(wide)], axis=1)
        g = dot(x, gate[...])
        u = dot(x, up[...])
        hidden = (g / (1.0 + jnp.exp(-g)) * u).astype(BF16)
        for t in range(out.shape[0]):
            out[t, part, :] = hidden


def down_kernel(place, hidden, *rest):
    downs, out = rest[:-1], rest[-1]
    parts, tall, length = out.shape[0], out.shape[1], out.shape[2]
    x = jnp.concatenate([hidden[t] for t in range(hidden.shape[0])], axis=1)
    result = dot(x, jnp.concatenate([down[...] for down in downs], axis=1)).astype(BF16)
    width = out.shape[3]
    for k in range(tall):
        to = (place[4] + (tall - k)) % tall
        for c in range(parts):
            rows = slice(c * length, (c + 1) * length)
            out[c, to] = result[rows, k * width : (k + 1) * width]


def gathered_sum_kernel(order, partial, out):
    parts, wide = partial.shape[0], partial.shape[1]
    sums = []
    for c in range(parts):
        total = partial[c, 0].astype(F32)
        for t in range(1, wide):
            total = total + partial[c, t].astype(F32)
        sums.append(total.astype(BF16))
    out[...] = dot(order[...], jnp.concatenate(sums, axis=0), 0, 0).astype(BF16)


def final_kernel(place, returned, slots, route_weight, output_weight, shared_down, *rest):
    both, (attended, combined) = rest[:-2], rest[-2:]
    tokens, width = slots.shape[1], returned.shape[1]
    routed = jnp.zeros((tokens, width), F32)
    for k in range(slots.shape[0]):
        hot = one_hot(slots, k, returned.shape[0]).astype(BF16)
        scale = jnp.broadcast_to(route_weight[k : k + 1, :], (width, tokens)).T
        routed = routed + dot(hot, returned[...], 0, 0) * scale
    tall, across = len(both), both[0].shape[0]
    units = both[0].shape[1] - VALUE
    heads, hidden, heads_weight, hidden_weight = [], [], [], []
    for a in range(tall):
        for b in range(across):
            at = (place[4] + (tall - a)) % tall * across + (place[5] + (across - b)) % across
            heads.append(both[a][b, 0:VALUE, :])
            hidden.append(both[a][b, VALUE:, :])
            heads_weight.append(output_weight[pl.ds(pl.multiple_of(at * VALUE, VALUE), VALUE), :])
            hidden_weight.append(shared_down[pl.ds(pl.multiple_of(at * units, units), units), :])
    joined = [jnp.concatenate(p, axis=0) for p in (heads, heads_weight, hidden, hidden_weight)]
    attended[...] = dot(joined[0], joined[1], 0, 0).astype(BF16)
    combined[...] = (dot(joined[2], joined[3], 0, 0) + routed).astype(BF16)


def tables(positions, width):
    inverse = (1.0 / 10000.0 ** (np.arange(0, ROTARY, 2) / ROTARY)).astype(np.float32)
    angles = inverse[:, None] * np.arange(positions, dtype=np.float32)[None, :]
    angles = angles.astype(np.float64).reshape(ROTARY // 2, positions // width, width)
    angles = angles.transpose(1, 0, 2)
    return np.cos(angles).astype(np.float32), np.sin(angles).astype(np.float32)


def row_order(outer, inner, capacity):
    source = np.arange(outer * inner * capacity).reshape(outer, inner, capacity)
    source = source.transpose(1, 0, 2).reshape(-1)
    return np.eye(source.size, dtype=np.float32)[source]


def exchange(array, axes):
    return lax.all_to_all(array, axes, 0, 0, tiled=True)


def per_device(
    compressed_query,
    compressed_key_value,
    rotary_key,
    query_norm_scale,
    context_norm_scale,
    query_plain_weight,
    query_rotary_weight,
    key_up_weight,
    value_up_weight,
    output_weight,
    mixture_input,
    mixture_gain,
    routes,
    route_weight,
    expert_gate,
    expert_up,
    expert_down,
    shared_gate,
    shared_up,
    shared_down,
):
    tokens, model = mixture_input.shape
    planes, cores = lax.axis_size("z"), lax.axis_size("core")
    wide = lax.axis_size(TP)
    experts = planes * cores
    width = model // wide
    capacity = tokens * routes.shape[1] * 3 // (2 * experts)
    units = expert_gate.shape[2]
    shared_units = shared_gate.shape[1]
    tall, across = lax.axis_size("y"), lax.axis_size("x")
    row = lax.axis_index("y")
    place = jnp.stack(
        [
            lax.axis_index(EP),
            lax.axis_index("z"),
            lax.axis_index("core"),
            lax.axis_index(TP),
            row,
            lax.axis_index("x"),
        ]
    ).astype(jnp.int32)
    cos, sin = tables(tokens * experts, tokens)
    order = jnp.asarray(row_order(planes, cores, capacity), BF16)

    kv = call(
        key_value_kernel,
        shape((PLAIN + VALUE + ROTARY, tokens)),
        (
            compressed_key_value,
            context_norm_scale[None],
            key_up_weight.T,
            value_up_weight.T,
            rotary_key.T,
        ),
        limit=56,
    )
    all_kv = lax.all_gather(kv, EP, axis=0, tiled=True).reshape(experts, *kv.shape)

    band = across * units
    downs = []
    for k in range(tall):
        part = lax.dynamic_slice_in_dim(expert_down[0], (row + k) % tall * band, band, 0)
        if k:
            part = lax.ppermute(part, "y", [(y, (y + k) % tall) for y in range(tall)])
        downs.append(part)

    sent, slots, shared, _ = call(
        functools.partial(dispatch_kernel, experts=experts, capacity=capacity),
        (
            shape((experts * capacity, width)),
            shape((routes.shape[1], tokens), jnp.int32),
            shape((shared_units, tokens)),
            shape((tokens, model)),
        ),
        (place, mixture_input, mixture_gain[None], routes.T, shared_gate.T, shared_up.T),
        smem=1,
        limit=12,
    )
    query = call(
        query_kernel,
        shape((tokens, PLAIN + 6 * ROTARY)),
        (
            place,
            compressed_query,
            query_norm_scale[None],
            query_plain_weight.T,
            query_rotary_weight.T,
            cos,
            sin,
        ),
        smem=1,
    )

    moved = exchange(sent.reshape(planes, cores * capacity, width), "z")
    rows = planes * capacity
    moved = call(
        order_kernel,
        shape((experts * capacity, width)),
        (order, moved.reshape(experts * capacity, width)),
    )
    moved = exchange(moved.reshape(cores, rows, width), "core")
    spread = call(
        spread_kernel,
        shape((wide, cores * rows, width)),
        (moved.reshape(cores * rows, width),),
    )
    arrived = exchange(spread, TP)
    hidden = call(
        functools.partial(hidden_kernel, parts=cores),
        shape((across, cores * rows, units)),
        (arrived, expert_gate[0], expert_up[0]),
        limit=14,
    )
    hidden = exchange(hidden, "x")
    partial = call(
        down_kernel,
        shape((cores, tall, rows, width)),
        (place, hidden, *downs),
        smem=1,
        limit=10,
    )
    parts = exchange(partial.reshape(cores * tall, rows, width), ("core", "y"))
    summed = call(
        gathered_sum_kernel,
        shape((experts * capacity, width)),
        (order, parts.reshape(cores, tall, rows, width)),
    )
    returned = exchange(summed.reshape(planes, cores * capacity, width), "z")

    both = call(
        attention_kernel,
        shape((1, VALUE + shared_units, tokens)),
        (query, all_kv, shared, cos, sin),
        scratch=[pltpu.VMEM((tokens, tokens * experts), F32)],
        limit=12,
    )
    pieces = [both]
    for k in range(1, across):
        pieces.append(lax.ppermute(both, "x", [(x, (x + k) % across) for x in range(across)]))
    both = jnp.concatenate(pieces, axis=0)
    pieces = [both]
    for k in range(1, tall):
        pieces.append(lax.ppermute(both, "y", [(y, (y + k) % tall) for y in range(tall)]))
    return call(
        final_kernel,
        (shape((tokens, width)), shape((tokens, width))),
        (
            place,
            returned.reshape(experts * capacity, width),
            slots,
            route_weight.T,
            output_weight,
            shared_down,
            *pieces,
        ),
        smem=1,
    )


def solution(mesh):
    split = Mesh(mesh.devices.reshape(16, 2, 4, 4), ("z", "core", "y", "x"))
    placed = (
        P(EP, None),
        P(EP, None),
        P(EP, None),
        P(),
        P(),
        P(None, TP),
        P(None, TP),
        P(None, TP),
        P(None, TP),
        P(None, TP),
        P(EP, None),
        P(),
        P(EP, None),
        P(EP, None),
        P(EP, None, TP),
        P(EP, None, TP),
        P(EP, None, TP),
        P(None, TP),
        P(None, TP),
        P(None, TP),
    )

    return jax.shard_map(
        per_device,
        mesh=split,
        in_specs=placed,
        out_specs=(P(EP, TP), P(EP, TP)),
        check_vma=False,
    )
```
